32 devices in a mesh: ep: 8 (over z, x), tp: 4 (over y, core).
Axes of the slice: x: 2, y: 2, z: 4, core: 2. Of those that a mesh axis runs over, the one named last changes fastest.
Arguments:
- tokens: bfloat16 [384, 1024], P('ep'), may hold values from -6 to 6
- head_state: float32 [384, 8, 64, 64], P('ep', 'tp'), may hold values from -6 to 6
- recept_weight: bfloat16 [1024, 512], P(None, 'tp'), may hold values from -0.1875 to 0.1875
- key_weight: bfloat16 [1024, 512], P(None, 'tp'), may hold values from -0.1875 to 0.1875
- value_weight: bfloat16 [1024, 512], P(None, 'tp'), may hold values from -0.1875 to 0.1875
- decay_down_factor: bfloat16 [1024, 64], replicated, may hold values from -0.1875 to 0.1875
- decay_up_factor: bfloat16 [64, 512], P(None, 'tp'), may hold values from -0.75 to 0.75
- decay_base: float32 [512], P('tp'), may hold values from -5 to 3
- rate_down_factor: bfloat16 [1024, 64], replicated, may hold values from -0.1875 to 0.1875
- rate_up_factor: bfloat16 [64, 512], P(None, 'tp'), may hold values from -0.75 to 0.75
- rate_base: float32 [512], P('tp'), may hold values from -3 to 3
- head_gain: float32 [512], P('tp'), may hold values from 0.1 to 1.9
- out_weight: bfloat16 [512, 1024], P('tp'), may hold values from -0.25 to 0.25
- route_experts: int32 [384, 4], P('ep'), may hold values from 0 to 7, all different within a row; in each aligned block of 48 rows (0 to 47, 48 to 95, ...) at most 48 rows name the same one
- route_weights: float32 [384, 4], P('ep'), may hold values from 0.03 to 0.2
- expert_gate: bfloat16 [8, 1024, 1024], P('ep', None, 'tp'), may hold values from -1 to 1
- expert_up: bfloat16 [8, 1024, 1024], P('ep', None, 'tp'), may hold values from -1 to 1
- expert_down: bfloat16 [8, 1024, 1024], P('ep', 'tp'), may hold values from -0.1875 to 0.1875
Outputs:
- layer_out: bfloat16 [384, 1024], P('ep', 'tp')
- new_state: float32 [384, 8, 64, 64], P('ep', 'tp')
The draws below stay inside these ranges and needn't reach their ends.
Inputs may be any that keep to these rules, and one draw needn't show every extreme that they name: `route_experts`: each row names 4 different experts. In each aligned block of 48 rows no expert is named by more than 48 rows, a bound that some block reaches.
All inputs are finite; a program needn't handle non-finite values.
Results may differ from the reference program's by a relative error of at most 0.02.
Values may be sent and summed in bfloat16 or wider, within the bound.
A program may use at most 128 MiB of HBM per device.

```python
import math
import jax
import jax.numpy as jnp
import numpy as np
from jax import lax

MODEL_DIMENSION = 1024
ALL_HEADS_WIDTH = 512
HEAD_DIM = 64
HEADS = 8
LOW_RANK_WIDTH = 64
DE = 1024
TOP_K = 4
SEQ_DEV = 48
SEQS = 384
EXPERTS = 8
CAP = 48
N_EP = 8
N_TP = 4


def column_scaled(key, stream):
    folded = jax.random.fold_in(key, stream)
    entries = jax.random.truncated_normal(jax.random.fold_in(folded, 1), -6.0, 6.0, (EXPERTS, MODEL_DIMENSION, DE), jnp.float32)
    column_scale = jnp.exp(jax.random.uniform(jax.random.fold_in(folded, 2), (EXPERTS, 1, DE), jnp.float32) * math.log(8.0))
    return jnp.clip(entries * column_scale / math.sqrt(MODEL_DIMENSION), -1.0, 1.0).astype(jnp.bfloat16)


def draw_expert_gate(key, part):
    return column_scaled(key, 11)


def draw_expert_up(key, part):
    return column_scaled(key, 23)


def block_levels(rng, shape, pieces, smallest, high):
    loudness, own = 1.0, jax.random.fold_in(rng, 6)
    for position, shards_of in pieces:
        heights = jnp.exp(jax.random.uniform(jax.random.fold_in(own, position), (shards_of,), jnp.float32, smallest / len(pieces), high / len(pieces)))
        loudness = loudness * jnp.repeat(heights, shape[position] // shards_of).reshape([-1 if axis == position else 1 for axis in range(len(shape))])
    return loudness


def shared_out(key, own, number, rows, count, top, bound, lean):
    sequence = jax.random.permutation(key, count)
    crowded, usual = load_shares(count, rows * top, bound, lean, True), load_shares(count, rows * top, bound, lean, False)
    places = jnp.arange(count)

    def named(sizes, offset_by):
        used = int((sizes > 0).sum())
        fixed = max(1, used // 4)
        moved = fixed + (places - fixed + offset_by * (used - fixed)) % max(1, count - fixed)
        return jnp.zeros((count,), jnp.int32).at[sequence[jnp.where(places < fixed, places, moved)]].set(jnp.asarray(sizes, jnp.int32))

    sizes = jnp.where(number % 4 == 0, named(crowded, number // 4), named(usual, number - number // 4 - 1))
    mixed = jax.random.permutation(jax.random.fold_in(own, 3), count)
    source_of, sink = mixed[0:count // 2 * 2:2], mixed[1:count // 2 * 2:2]
    slack = jnp.minimum(sizes[source_of] - 1, bound - sizes[sink]) // 2
    slack = jnp.where((source_of == sequence[0]) | (sink == sequence[0]) | (sizes[sink] == 0), 0, jnp.maximum(slack, 0))
    moved = jax.random.randint(jax.random.fold_in(own, 4), (count // 2,), 0, 1 << 20) % (slack + 1)
    sizes = sizes.at[source_of].add(-moved).at[sink].add(moved)
    labels = jnp.searchsorted(jnp.cumsum(sizes), jnp.arange(rows * top), side="right").astype(jnp.int32)
    grid = labels.reshape(top, rows).T
    grid = grid[jax.random.permutation(jax.random.fold_in(own, 1), rows)]
    offset_by = jax.random.randint(jax.random.fold_in(own, 2), (rows, 1), 0, top)
    return jnp.take_along_axis(grid, (jnp.arange(top)[None, :] + offset_by) % top, axis=1)


def load_shares(number_of, total, most, lean, full):
    weights = [(1 << 20) // math.isqrt(grade ** lean) + 1 for grade in range(1, number_of + 1)]
    largest = most if full else min(most, max(-(-total // number_of), total * weights[0] // sum(weights)))
    least = 1 if total - largest >= number_of - 1 else 0
    counts, rest = [largest] + [least] * (number_of - 1), total - largest - least * (number_of - 1)
    while rest > 0:
        movable = [i for i in range(1, number_of) if counts[i] < largest] or [i for i in range(1, number_of) if counts[i] < most]
        mass, budget = sum([weights[i] for i in movable]), rest
        for i in movable:
            addition = min(most - counts[i], max(1, budget * weights[i] // mass), rest)
            counts[i] = counts[i] + addition
            rest = rest - addition
    return np.array(counts)


def gaussian(own_key, dims, scale, bound, cuts=(), kind=jnp.bfloat16):
    result = jax.random.normal(own_key, dims, jnp.float32) * scale
    if len(cuts) > 0:
        result = block_levels(own_key, dims, cuts, -0.22, 0.18) * result
    return jnp.clip(result, min=-bound, max=bound).astype(kind)


def setup_inputs(seed: int = 0) -> dict:
    arg_keys = jax.random.split(jax.random.key(seed), 19)
    tokens = gaussian(arg_keys[0], (SEQS, MODEL_DIMENSION), 1.0, 6.0, ((0, 8),))
    head_state = gaussian(arg_keys[1], (SEQS, HEADS, HEAD_DIM, HEAD_DIM), 1.0, 6.0, ((0, 8), (1, 4)), jnp.float32)
    recept_weight = gaussian(arg_keys[2], (MODEL_DIMENSION, ALL_HEADS_WIDTH), MODEL_DIMENSION ** -0.5, 0.1875, ((1, 4),))
    key_weight = gaussian(arg_keys[3], (MODEL_DIMENSION, ALL_HEADS_WIDTH), MODEL_DIMENSION ** -0.5, 0.1875, ((1, 4),))
    value_weight = gaussian(arg_keys[4], (MODEL_DIMENSION, ALL_HEADS_WIDTH), MODEL_DIMENSION ** -0.5, 0.1875, ((1, 4),))
    decay_down_factor = gaussian(arg_keys[5], (MODEL_DIMENSION, LOW_RANK_WIDTH), MODEL_DIMENSION ** -0.5, 0.1875)
    decay_up_factor = gaussian(arg_keys[6], (LOW_RANK_WIDTH, ALL_HEADS_WIDTH), LOW_RANK_WIDTH ** -0.5, 0.75, ((1, 4),))
    decay_base = jnp.clip(-5.0 + 8.0 * jax.random.uniform(arg_keys[7], (ALL_HEADS_WIDTH,), jnp.float32) ** block_levels(arg_keys[7], (ALL_HEADS_WIDTH,), ((0, 4),), -0.2, 0.2), -5.0, 3.0)
    rate_down_factor = gaussian(arg_keys[8], (MODEL_DIMENSION, LOW_RANK_WIDTH), MODEL_DIMENSION ** -0.5, 0.1875)
    rate_up_factor = gaussian(arg_keys[9], (LOW_RANK_WIDTH, ALL_HEADS_WIDTH), LOW_RANK_WIDTH ** -0.5, 0.75, ((1, 4),))
    rate_base = jnp.clip(jax.random.uniform(arg_keys[10], (ALL_HEADS_WIDTH,), jnp.float32, -3.0, 3.0) * block_levels(arg_keys[10], (ALL_HEADS_WIDTH,), ((0, 4),), -0.4, 0.0), -3.0, 3.0)
    head_gain = jnp.clip(1.0 + 0.18 * jax.random.normal(arg_keys[11], (ALL_HEADS_WIDTH,), jnp.float32), 0.1, 1.9)
    out_weight = gaussian(arg_keys[12], (ALL_HEADS_WIDTH, MODEL_DIMENSION), ALL_HEADS_WIDTH ** -0.5, 0.25, ((0, 4),))
    route_experts_keys = jax.random.split(jax.random.fold_in(arg_keys[13], 1), SEQS // SEQ_DEV)
    route_experts_turns = jax.random.permutation(jax.random.fold_in(arg_keys[13], 3), SEQS // SEQ_DEV)
    route_experts = jax.vmap(lambda own, number: shared_out(jax.random.fold_in(arg_keys[13], 2), own, number, SEQ_DEV, EXPERTS, TOP_K, CAP, 2))(route_experts_keys, route_experts_turns).reshape((SEQS, TOP_K))
    route_weights = jnp.clip(jnp.exp(math.log(0.2) - 1.89712 * jax.random.uniform(arg_keys[14], (SEQS, TOP_K), jnp.float32) ** block_levels(arg_keys[14], (SEQS, TOP_K), ((0, 8),), -0.2, 0.2)), 0.03, 0.2)
    expert_gate = draw_expert_gate(jax.random.fold_in(arg_keys[18], 71), 0)
    expert_up = draw_expert_up(jax.random.fold_in(arg_keys[18], 71), 0)
    expert_down = gaussian(arg_keys[17], (EXPERTS, DE, MODEL_DIMENSION), DE ** -0.5, 0.1875, ((0, 8), (1, 4)))
    return dict(tokens=tokens, head_state=head_state, recept_weight=recept_weight, key_weight=key_weight, value_weight=value_weight, decay_down_factor=decay_down_factor, decay_up_factor=decay_up_factor, decay_base=decay_base, rate_down_factor=rate_down_factor, rate_up_factor=rate_up_factor, rate_base=rate_base, head_gain=head_gain, out_weight=out_weight, route_experts=route_experts, route_weights=route_weights, expert_gate=expert_gate, expert_up=expert_up, expert_down=expert_down)


NORM_EPS = 1e-05
GROUP_EPS = 0.00064
UNIT_EPS = 1e-06
CLAMP_LIMIT = 7.0
GLU_ALPHA = 1.702

def row_norm(values):
    return values * lax.rsqrt(lax.optimization_barrier(jnp.mean(values * values, axis=-1, keepdims=True)) + NORM_EPS)

def clamped_unit(gate_pre, up_pre):
    gated = jnp.minimum(gate_pre, CLAMP_LIMIT)
    linear = jnp.clip(up_pre, -CLAMP_LIMIT, CLAMP_LIMIT)
    return gated * jax.nn.sigmoid(GLU_ALPHA * gated) * (linear + 1.0)

def update_heads(head_state, recept, keys, values, decay_rate, rate_gate, head_gain):
    seq_count, head_count, head_size = head_state.shape[:3]

    def by_heads(operand):
        return operand.astype(jnp.float32).reshape(seq_count, head_count, head_size)
    recept_heads = by_heads(recept)
    key_heads = by_heads(keys)
    value_heads = by_heads(values)
    decay_heads = by_heads(decay_rate)
    rate_heads = by_heads(rate_gate)
    unit_key = key_heads * lax.rsqrt(lax.optimization_barrier(jnp.sum(key_heads * key_heads, axis=-1, keepdims=True)) + UNIT_EPS)
    highest = lax.Precision.HIGHEST
    state_unit = jnp.einsum('shvk,shk->shv', head_state, unit_key, precision=highest)
    new_state = head_state * decay_heads[:, :, None, :] - state_unit[..., None] * (unit_key * rate_heads)[:, :, None, :] + value_heads[..., None] * (key_heads * rate_heads)[:, :, None, :]
    head_out = jnp.einsum('shvk,shk->shv', new_state, recept_heads, precision=highest)
    centre = lax.optimization_barrier(jnp.mean(head_out, axis=-1, keepdims=True))
    spread = lax.optimization_barrier(jnp.mean(jnp.square(head_out - centre), axis=-1, keepdims=True))
    normed_heads = (head_out - centre) * lax.rsqrt(spread + GROUP_EPS)
    mixed = (normed_heads.reshape(seq_count, -1) * head_gain).astype(jnp.bfloat16)
    return (new_state, mixed)

def reference(tokens, head_state, recept_weight, key_weight, value_weight, decay_down_factor, decay_up_factor, decay_base, rate_down_factor, rate_up_factor, rate_base, head_gain, out_weight, route_experts, route_weights, expert_gate, expert_up, expert_down):
    tokens_float = tokens.astype(jnp.float32)
    normed = row_norm(tokens_float).astype(jnp.bfloat16)
    recept = jnp.dot(normed, recept_weight, preferred_element_type=jnp.float32).astype(jnp.bfloat16)
    keys = jnp.dot(normed, key_weight, preferred_element_type=jnp.float32).astype(jnp.bfloat16)
    values = jnp.dot(normed, value_weight, preferred_element_type=jnp.float32).astype(jnp.bfloat16)
    decay_low = jnp.tanh(jnp.dot(normed, decay_down_factor, preferred_element_type=jnp.float32)).astype(jnp.bfloat16)
    rate_low = jnp.dot(normed, rate_down_factor, preferred_element_type=jnp.float32).astype(jnp.bfloat16)
    decay_pre = decay_base + jnp.dot(decay_low, decay_up_factor, preferred_element_type=jnp.float32)
    decay_rate = jnp.exp(-jnp.exp(-jax.nn.softplus(-decay_pre) - 0.5))
    rate_gate = jax.nn.sigmoid(rate_base + jnp.dot(rate_low, rate_up_factor, preferred_element_type=jnp.float32))
    new_state, mixed = update_heads(head_state, recept, keys, values, decay_rate, rate_gate, head_gain)
    group_width = ALL_HEADS_WIDTH // N_TP
    partials = jnp.einsum('sgr,grd->gsd', mixed.reshape(SEQS, N_TP, group_width).astype(jnp.float32), out_weight.reshape(N_TP, group_width, MODEL_DIMENSION).astype(jnp.float32))
    partials = lax.optimization_barrier(partials.astype(jnp.bfloat16)).astype(jnp.float32)
    residual = (tokens_float + lax.optimization_barrier(jnp.sum(partials, axis=0))).astype(jnp.bfloat16)
    expert_input = row_norm(residual.astype(jnp.float32)).astype(jnp.bfloat16)
    grouped = route_experts.reshape(N_EP, SEQ_DEV * TOP_K)
    onehot = (grouped[:, :, None] == jnp.arange(EXPERTS, dtype=jnp.int32)[None, None, :]).astype(jnp.int32)
    earlier = jnp.cumsum(onehot, axis=1) - onehot
    slot_rank = lax.optimization_barrier(jnp.sum(earlier * onehot, axis=-1)).astype(jnp.int32)
    target = (grouped * CAP + slot_rank).astype(jnp.int32)
    repeated = jnp.repeat(expert_input.reshape(N_EP, SEQ_DEV, MODEL_DIMENSION), TOP_K, axis=1)
    sources = jnp.arange(N_EP, dtype=jnp.int32)[:, None]
    buffer = jnp.zeros((N_EP, EXPERTS * CAP, MODEL_DIMENSION), jnp.bfloat16).at[sources, target].set(repeated)
    per_expert = buffer.reshape(N_EP, EXPERTS, CAP, MODEL_DIMENSION).transpose(1, 0, 2, 3).reshape(EXPERTS, N_EP * CAP, MODEL_DIMENSION)
    hidden_group = DE // N_TP

    def one_expert(operands):
        slot_rows, gate_matrix, up_matrix, down_matrix = operands
        gate_pre = jnp.dot(slot_rows, gate_matrix, preferred_element_type=jnp.float32)
        up_pre = jnp.dot(slot_rows, up_matrix, preferred_element_type=jnp.float32)
        activated = clamped_unit(gate_pre, up_pre).astype(jnp.bfloat16)
        expert_parts = jnp.einsum('rgc,gcd->grd', activated.reshape(-1, N_TP, hidden_group).astype(jnp.float32), down_matrix.reshape(N_TP, hidden_group, MODEL_DIMENSION).astype(jnp.float32))
        expert_parts = lax.optimization_barrier(expert_parts.astype(jnp.bfloat16)).astype(jnp.float32)
        return lax.optimization_barrier(jnp.sum(expert_parts, axis=0)).astype(jnp.bfloat16)
    results = lax.map(one_expert, (per_expert, expert_gate, expert_up, expert_down))
    returned = results.reshape(EXPERTS, N_EP, CAP, MODEL_DIMENSION).transpose(1, 0, 2, 3).reshape(N_EP, EXPERTS * CAP, MODEL_DIMENSION)
    picked = jnp.take_along_axis(returned, target[:, :, None], axis=1)
    picked = picked.reshape(SEQS, TOP_K, MODEL_DIMENSION).astype(jnp.float32)
    mixture = lax.optimization_barrier(jnp.sum(route_weights[:, :, None] * picked, axis=1))
    layer_out = (residual.astype(jnp.float32) + mixture).astype(jnp.bfloat16)
    return (layer_out, new_state)
```

```python
import functools

import jax
import jax.numpy as jnp
from jax import lax
from jax.experimental import pallas as pl
from jax.experimental.pallas import tpu as pltpu
from jax.sharding import PartitionSpec as P

NORM_EPS = 1e-05
GROUP_EPS = 0.00064
UNIT_EPS = 1e-06
CLAMP_LIMIT = 7.0
GLU_ALPHA = 1.702


MESH = pl.DeviceIdType.MESH
VMEM = pltpu.MemorySpace.VMEM


def row_norm(values):
    return values * lax.rsqrt(jnp.mean(values * values, axis=-1, keepdims=True) + NORM_EPS)


def clamped_unit(gate_pre, up_pre):
    gated = jnp.minimum(gate_pre, CLAMP_LIMIT)
    linear = jnp.clip(up_pre, -CLAMP_LIMIT, CLAMP_LIMIT)
    return gated * jax.nn.sigmoid(GLU_ALPHA * gated) * (linear + 1.0)


def heads_kernel(rows_per_step, input_count, *refs):
    state, inputs = refs[0], refs[1 : 1 + input_count]
    new_state, mixed, held = refs[1 + input_count : 4 + input_count]
    copies = refs[4 + input_count : 4 + 2 * input_count]
    input_sem, load_sem, store_sem, decay_rows, unit_rows, key_rows = refs[
        4 + 2 * input_count : 10 + 2 * input_count
    ]
    value_rows, recept_rows, head_rows = refs[10 + 2 * input_count :]
    seq_count, head_count, head_size = state.shape[:3]
    steps = seq_count // rows_per_step

    def chunk(step):
        return pl.ds(step * rows_per_step, rows_per_step)

    def load(step):
        return pltpu.make_async_copy(
            state.at[chunk(step)], held.at[chunk(step)], load_sem.at[step]
        )

    def store(step):
        return pltpu.make_async_copy(
            held.at[chunk(step)], new_state.at[chunk(step)], store_sem.at[step]
        )

    staged = [
        pltpu.make_async_copy(source, target, input_sem.at[index])
        for index, (source, target) in enumerate(zip(inputs, copies))
    ]
    for copy in staged:
        copy.start()
    for copy in staged:
        copy.wait()
    for step in range(steps):
        load(step).start()
    (
        tokens,
        recept_weight,
        key_weight,
        value_weight,
        decay_down,
        decay_up,
        decay_base,
        rate_down,
        rate_up,
        rate_base,
        gain,
    ) = copies
    normed = row_norm(tokens[...].astype(jnp.float32)).astype(jnp.bfloat16)

    def product(left, right):
        return jnp.dot(left, right[...], preferred_element_type=jnp.float32)

    def turned(left, right):
        return lax.dot_general(
            left, right, (((1,), (1,)), ((), ())), preferred_element_type=jnp.float32
        )

    def rounded(value):
        return value.astype(jnp.bfloat16)

    recept = rounded(product(normed, recept_weight)).astype(jnp.float32)
    keys = rounded(product(normed, key_weight)).astype(jnp.float32)
    values = rounded(product(normed, value_weight)).astype(jnp.float32)
    decay_low = rounded(jnp.tanh(turned(normed, decay_down[...])))
    rate_low = rounded(turned(normed, rate_down[...]))
    decay_pre = decay_base[...] + product(decay_low, decay_up)
    softplus = jnp.maximum(-decay_pre, 0.0) + jnp.log(1.0 + jnp.exp(-jnp.abs(decay_pre)))
    decay = jnp.exp(-jnp.exp(-softplus - 0.5))
    rate = jax.nn.sigmoid(rate_base[...] + product(rate_low, rate_up))
    for head in range(head_count):
        lanes = slice(head * head_size, (head + 1) * head_size)
        head_keys = keys[:, lanes]
        scale = lax.rsqrt(jnp.sum(head_keys * head_keys, axis=-1, keepdims=True) + UNIT_EPS)
        decay_rows[head] = decay[:, lanes]
        unit_rows[head] = head_keys * scale * scale
        key_rows[head] = head_keys * rate[:, lanes]
        value_rows[head] = values[:, lanes]
        recept_rows[head] = recept[:, lanes]

    shape = (head_size, head_size)
    diagonal = lax.broadcasted_iota(jnp.int32, shape, 0) == lax.broadcasted_iota(jnp.int32, shape, 1)
    ones = jnp.ones(shape, jnp.bfloat16)
    places = lax.broadcasted_iota(jnp.int32, (rows_per_step, head_size), 0)
    width = next(each for each in (4, 2, 1) if rows_per_step % each == 0)

    def advance(step, _):
        load(step).wait()
        for head in range(head_count):
            queries = rounded(recept_rows[head, chunk(step), :])
            total = jnp.zeros((rows_per_step, head_size), jnp.float32)
            for first in range(0, rows_per_step, width):
                seqs = [step * rows_per_step + first + each for each in range(width)]
                olds = [held[seq, head] for seq in seqs]
                pulled = []
                for seq, old in zip(seqs, olds):
                    row = pl.ds(seq, 1)
                    wanted = jnp.where(diagonal, value_rows[head, row, :], 0.0)
                    pulled.append(rounded(wanted - old * unit_rows[head, row, :]))
                columns = product(jnp.concatenate(pulled, axis=0), ones)
                blocks = []
                for each, (seq, old) in enumerate(zip(seqs, olds)):
                    row = pl.ds(seq, 1)
                    column = columns[each * head_size : (each + 1) * head_size]
                    fresh = old * decay_rows[head, row, :] + column * key_rows[head, row, :]
                    held[seq, head] = fresh
                    blocks.append(rounded(fresh * recept_rows[head, row, :]))
                outs = product(jnp.concatenate(blocks, axis=0), ones)
                for each, seq in enumerate(seqs):
                    part = outs[each * head_size : (each + 1) * head_size]
                    part = jnp.sum(jnp.where(diagonal, part, 0.0), axis=0, keepdims=True)
                    head_rows[head, pl.ds(seq, 1), :] = part
        store(step).start()
        return 0

    lax.fori_loop(0, steps, advance, 0)
    wide = []
    for head in range(head_count):
        outs = head_rows[head]
        centred = outs - jnp.mean(outs, axis=-1, keepdims=True)
        spread = jnp.mean(centred * centred, axis=-1, keepdims=True)
        lanes = slice(head * head_size, (head + 1) * head_size)
        wide.append(centred * lax.rsqrt(spread + GROUP_EPS) * gain[:, lanes])
    mixed[...] = rounded(jnp.concatenate(wide, axis=-1))
    for step in range(steps):
        store(step).wait()


def in_hbm(value):
    return pltpu.with_memory_space_constraint(value, pltpu.MemorySpace.HBM)


def run_heads(tokens, head_state, *parameters):
    seq_count, head_count, head_size = head_state.shape[:3]
    rows_per_step = 8 if seq_count % 8 == 0 else seq_count
    inputs = [tokens] + [each.reshape(1, -1) if each.ndim == 1 else each for each in parameters]

    rows = (head_count, seq_count, head_size)
    mixed = (seq_count, head_count * head_size)
    anywhere = pl.BlockSpec(memory_space=pltpu.MemorySpace.HBM)
    steps = seq_count // rows_per_step
    dma = pltpu.SemaphoreType.DMA
    return pl.pallas_call(
        functools.partial(heads_kernel, rows_per_step, len(inputs)),
        in_specs=[anywhere] * (1 + len(inputs)),
        out_specs=[anywhere, pl.BlockSpec(memory_space=VMEM)],
        out_shape=[
            pltpu.MemorySpace.HBM(head_state.shape, jnp.float32),
            VMEM(mixed, jnp.bfloat16),
        ],
        scratch_shapes=[pltpu.VMEM(head_state.shape, jnp.float32)]
        + [pltpu.VMEM(each.shape, each.dtype) for each in inputs]
        + [dma((len(inputs),)), dma((steps,)), dma((steps,))]
        + [pltpu.VMEM(rows, jnp.float32)] * 6,
        compiler_params=pltpu.CompilerParams(vmem_limit_bytes=40 * 2**20),
        name="heads",
    )(*map(in_hbm, [head_state] + inputs))


def flipped(index, mask):
    bit = 1
    result = index
    while bit <= mask:
        if mask & bit:
            result = result + bit * (1 - 2 * ((index // bit) % 2))
        bit *= 2
    return result


def experts_kernel(
    n_ep,
    n_tp,
    mixed,
    out_weight,
    tokens,
    routes,
    weights,
    gate_hbm,
    up_hbm,
    down_hbm,
    layer_out,
    gate,
    up,
    down,
    shares,
    got_shares,
    rows,
    parts,
    leaving,
    arriving,
    homeward,
    returned,
    weight_sem,
    share_send,
    share_recv,
    spread_send,
    rows_send,
    rows_recv,
    part_send,
    part_recv,
    home_send,
    home_recv,
):
    me_ep, me_tp = lax.axis_index("ep"), lax.axis_index("tp")
    seq_count = tokens.shape[0]
    columns = shares.shape[2]
    levels = n_tp.bit_length() - 1

    barrier = pltpu.get_barrier_semaphore()
    for mask in range(1, n_tp):
        pl.semaphore_signal(
            barrier, inc=1, device_id={"tp": flipped(me_tp, mask)}, device_id_type=MESH
        )
    for mask in range(1, n_ep):
        pl.semaphore_signal(
            barrier, inc=1, device_id={"ep": flipped(me_ep, mask)}, device_id_type=MESH
        )
    loads = [
        pltpu.make_async_copy(source.at[0], target, weight_sem.at[index])
        for index, (source, target) in enumerate(((gate_hbm, gate), (up_hbm, up), (down_hbm, down)))
    ]
    for load in loads:
        load.start()
    started = []

    def send(source, target, send_sem, recv_sem, device):
        copy = pltpu.make_async_remote_copy(
            src_ref=source,
            dst_ref=target,
            send_sem=send_sem,
            recv_sem=recv_sem,
            device_id=device,
            device_id_type=MESH,
        )
        copy.start()
        started.append(copy)
        return copy

    projected = jnp.dot(mixed[...], out_weight[...], preferred_element_type=jnp.float32)
    for part in range(n_tp):
        shares[part] = projected[:, part * columns : (part + 1) * columns].astype(jnp.bfloat16)
    pl.semaphore_wait(barrier, n_tp + n_ep - 2)

    incoming = [
        send(
            shares.at[flipped(me_tp, mask)],
            got_shares.at[mask - 1],
            share_send.at[mask - 1],
            share_recv.at[mask - 1],
            {"tp": flipped(me_tp, mask)},
        )
        for mask in range(n_tp - 1, 0, -1)
    ]
    own_columns = pl.ds(pl.multiple_of(me_tp * columns, columns), columns)
    summed = shares[me_tp].astype(jnp.float32)
    for copy in incoming:
        copy.wait_recv()
    for mask in range(1, n_tp):
        summed += got_shares[mask - 1].astype(jnp.float32)
    residual = (tokens[:, own_columns].astype(jnp.float32) + summed).astype(jnp.bfloat16)
    rows[0, 0] = residual

    got = {}
    for mask in range(n_ep - 1, 0, -1):
        got[mask, 0] = send(
            rows.at[0, 0],
            rows.at[mask, 0],
            spread_send.at[mask - 1],
            rows_recv.at[mask, 0],
            {"ep": flipped(me_ep, mask)},
        )

    def forward(mask, part, bit):
        got[mask, part + bit] = send(
            rows.at[mask, part],
            rows.at[mask, part + bit],
            rows_send.at[mask, part + bit],
            rows_recv.at[mask, part + bit],
            {"tp": flipped(me_tp, bit)},
        )

    bits = [1 << level for level in range(levels - 1, -1, -1)]
    for mask in range(n_ep):
        if mask:
            got[mask, 0].wait_recv()
        for bit in bits:
            forward(mask, 0, bit)

    def relay(masks):
        for top in bits[:-1]:
            for part in range(top, n_tp, 2 * top):
                for mask in masks:
                    got[mask, part].wait_recv()
                    for bit in bits:
                        if bit < top:
                            forward(mask, part, bit)

    near, far = range(n_ep // 2), range(n_ep // 2, n_ep)
    copies = {}

    def own(part):
        return pl.ds(pl.multiple_of(flipped(me_tp, part) * columns, columns), columns)

    def send_part(part, mask, bit):
        copies[part, mask] = send(
            leaving.at[part, mask],
            arriving.at[part, mask],
            part_send.at[part, mask],
            part_recv.at[part, mask],
            {"tp": flipped(me_tp, bit)},
        )

    def compute(masks):
        for mask in masks:
            for part in range(1, n_tp, 2):
                got[mask, part].wait_recv()
        span = slice(masks[0], masks[-1] + 1)
        total = len(masks) * seq_count
        squares = jnp.zeros((total, columns), jnp.float32)
        gate_pre = jnp.zeros((total, gate.shape[1]), jnp.float32)
        up_pre = jnp.zeros((total, up.shape[1]), jnp.float32)
        for part in range(n_tp):
            block = rows[span, part].reshape(total, columns)
            wide = block.astype(jnp.float32)
            squares += wide * wide
            gate_pre += jnp.dot(block, gate[own(part), :], preferred_element_type=jnp.float32)
            up_pre += jnp.dot(block, up[own(part), :], preferred_element_type=jnp.float32)
        mean = jnp.sum(squares, axis=-1, keepdims=True) / (n_tp * columns)
        scale = lax.rsqrt(mean + NORM_EPS)
        activated = clamped_unit(gate_pre * scale, up_pre * scale).astype(jnp.bfloat16)
        shape = (len(masks), seq_count, columns)
        for part in list(range(1, n_tp, 2)) + list(range(0, n_tp, 2)):
            value = jnp.dot(activated, down[:, own(part)], preferred_element_type=jnp.float32)
            if part % 2 == 0:
                parts[part, span] = value.reshape(shape)
                continue
            leaving[part, span] = value.astype(jnp.bfloat16).reshape(shape)
            for mask in reversed(masks):
                send_part(part, mask, 1)

    def fold(masks):
        for level in range(1, levels):
            bit = 1 << level
            for mask in reversed(masks):
                for part in range(n_tp - bit, -1, -bit):
                    before = part + bit // 2
                    copies[before, mask].wait_recv()
                    value = parts[part, mask] + arriving[before, mask].astype(jnp.float32)
                    if part % (2 * bit) == bit:
                        leaving[part, mask] = value.astype(jnp.bfloat16)
                        send_part(part, mask, bit)
                    else:
                        parts[part, mask] = value

    back = {}

    def home(masks):
        for mask in reversed(masks):
            last = n_tp // 2
            copies[last, mask].wait_recv()
            value = (parts[0, mask] + arriving[last, mask].astype(jnp.float32)).astype(jnp.bfloat16)
            if mask == 0:
                returned[0] = value
                continue
            homeward[mask - 1] = value
            back[mask] = send(
                homeward.at[mask - 1],
                returned.at[mask],
                home_send.at[mask - 1],
                home_recv.at[mask - 1],
                {"ep": flipped(me_ep, mask)},
            )

    relay(near)
    for load in loads:
        load.wait()
    compute(near)
    relay(far)
    fold(near)
    compute(far)
    fold(far)
    home(near)
    home(far)
    shape = (seq_count, seq_count)
    diagonal = lax.broadcasted_iota(jnp.int32, shape, 0) == lax.broadcasted_iota(jnp.int32, shape, 1)
    result = residual.astype(jnp.float32)
    for mask in range(n_ep):
        chosen = routes[...] == flipped(me_ep, mask)
        share = jnp.sum(jnp.where(chosen, weights[...], 0.0), axis=0, keepdims=True)
        share = jnp.sum(jnp.where(diagonal, share, 0.0), axis=-1, keepdims=True)
        if mask:
            back[mask].wait_recv()
        result += share * returned[mask].astype(jnp.float32)
    layer_out[...] = result
    for copy in started:
        copy.wait_send()


def run_experts(mixed, out_weight, tokens, routes, weights, gate, up, down):
    n_ep, n_tp = lax.axis_size("ep"), lax.axis_size("tp")
    seq_count, width = tokens.shape
    columns = width // n_tp
    block = (seq_count, columns)
    vmem = pl.BlockSpec(memory_space=VMEM)
    anywhere = pl.BlockSpec(memory_space=pl.ANY)
    dma = pltpu.SemaphoreType.DMA
    return pl.pallas_call(
        functools.partial(experts_kernel, n_ep, n_tp),
        in_specs=[vmem] * 5 + [anywhere] * 3,
        out_specs=vmem,
        out_shape=VMEM(block, jnp.float32),
        scratch_shapes=[
            pltpu.VMEM(gate.shape[1:], jnp.bfloat16),
            pltpu.VMEM(up.shape[1:], jnp.bfloat16),
            pltpu.VMEM(down.shape[1:], jnp.bfloat16),
            pltpu.VMEM((n_tp,) + block, jnp.bfloat16),
            pltpu.VMEM((n_tp - 1,) + block, jnp.bfloat16),
            pltpu.VMEM((n_ep, n_tp) + block, jnp.bfloat16),
            pltpu.VMEM((n_tp, n_ep) + block, jnp.float32),
            pltpu.VMEM((n_tp, n_ep) + block, jnp.bfloat16),
            pltpu.VMEM((n_tp, n_ep) + block, jnp.bfloat16),
            pltpu.VMEM((n_ep - 1,) + block, jnp.bfloat16),
            pltpu.VMEM((n_ep,) + block, jnp.bfloat16),
            dma((3,)),
            dma((n_tp - 1,)),
            dma((n_tp - 1,)),
            dma((n_ep - 1,)),
            dma((n_ep, n_tp)),
            dma((n_ep, n_tp)),
            dma((n_tp, n_ep)),
            dma((n_tp, n_ep)),
            dma((n_ep - 1,)),
            dma((n_ep - 1,)),
        ],
        compiler_params=pltpu.CompilerParams(collective_id=0, has_side_effects=True, vmem_limit_bytes=40 * 2**20),
        name="experts",
    )(mixed, *map(in_hbm, (out_weight, tokens, routes, weights, gate, up, down))).astype(jnp.bfloat16)


def every_row_fits(seq_count, top_count, width):
    n_ep, n_tp = lax.axis_size("ep"), lax.axis_size("tp")
    capacity = max(2, (2 * seq_count * top_count + n_ep - 1) // n_ep)
    powers = n_ep & (n_ep - 1) == 0 and n_tp & (n_tp - 1) == 0 and min(n_ep, n_tp) > 1
    aligned = seq_count % 16 == 0 and width % (128 * n_tp) == 0
    return capacity >= seq_count and powers and aligned


def local(
    tokens,
    head_state,
    recept_weight,
    key_weight,
    value_weight,
    decay_down_factor,
    decay_up_factor,
    decay_base,
    rate_down_factor,
    rate_up_factor,
    rate_base,
    head_gain,
    out_weight,
    route_experts,
    route_weights,
    expert_gate,
    expert_up,
    expert_down,
):
    new_state, mixed = run_heads(
        tokens,
        head_state,
        recept_weight,
        key_weight,
        value_weight,
        decay_down_factor.T,
        decay_up_factor,
        decay_base,
        rate_down_factor.T,
        rate_up_factor,
        rate_base,
        head_gain,
    )
    if every_row_fits(*route_experts.shape, tokens.shape[1]):
        layer_out = run_experts(
            mixed,
            out_weight,
            tokens,
            route_experts.T,
            route_weights.T,
            expert_gate,
            expert_up,
            expert_down,
        )
        return (layer_out, new_state)
    tokens_float = tokens.astype(jnp.float32)
    partial_value = jnp.dot(mixed, out_weight, preferred_element_type=jnp.float32).astype(
        jnp.bfloat16
    )
    partial_value = lax.optimization_barrier(partial_value).astype(jnp.float32)
    summed = lax.psum(partial_value.astype(jnp.bfloat16), "tp").astype(jnp.float32)
    residual = (tokens_float + summed).astype(jnp.bfloat16)
    expert_input = row_norm(residual.astype(jnp.float32)).astype(jnp.bfloat16)
    seq_count, top_count = route_experts.shape
    expert_count = lax.axis_size("ep")
    capacity = max(2, (2 * seq_count * top_count + expert_count - 1) // expert_count)
    column_count = expert_input.shape[1] // lax.axis_size("tp")
    column_start = lax.axis_index("tp") * column_count
    flat_routes = route_experts.reshape(-1)
    onehot = (flat_routes[:, None] == jnp.arange(expert_count, dtype=jnp.int32)[None, :]).astype(
        jnp.int32
    )
    earlier = jnp.cumsum(onehot, axis=0) - onehot
    target = flat_routes * capacity + jnp.sum(earlier * onehot, axis=1)
    slot_ids = jnp.arange(expert_count * capacity, dtype=jnp.int32)
    dispatch_map = jnp.any(
        slot_ids[:, None, None] == target.reshape(seq_count, top_count)[None], axis=-1
    )
    dispatch_map = dispatch_map.astype(jnp.bfloat16)
    outgoing = lax.dynamic_slice_in_dim(expert_input, column_start, column_count, 1)
    buffer = jnp.dot(dispatch_map, outgoing, preferred_element_type=jnp.float32).astype(
        jnp.bfloat16
    )
    buffer = buffer.reshape(expert_count, capacity, outgoing.shape[1])
    slot_rows = lax.all_gather(
        lax.all_to_all(buffer, "ep", split_axis=0, concat_axis=0, tiled=True),
        "tp",
        axis=2,
        tiled=True,
    )
    source_count, slot_count, model_width = slot_rows.shape
    flat_rows = slot_rows.reshape(-1, model_width)
    gate_pre = jnp.dot(flat_rows, expert_gate[0], preferred_element_type=jnp.float32)
    up_pre = jnp.dot(flat_rows, expert_up[0], preferred_element_type=jnp.float32)
    activated = clamped_unit(gate_pre, up_pre).astype(jnp.bfloat16)
    part_out = jnp.dot(activated, expert_down[0], preferred_element_type=jnp.float32).astype(
        jnp.bfloat16
    )
    part_out = lax.optimization_barrier(part_out).astype(jnp.float32)
    part_out = part_out.reshape(source_count, slot_count, model_width)
    shares = lax.psum_scatter(part_out.astype(jnp.bfloat16), "tp", scatter_dimension=2, tiled=True)
    returned = lax.all_to_all(shares, "ep", split_axis=0, concat_axis=0, tiled=True)
    picked = returned.reshape(expert_count * capacity, column_count)[target]
    picked = picked.reshape(seq_count, top_count, column_count).astype(jnp.float32)
    mixture = jnp.sum(route_weights[:, :, None] * picked, axis=1)
    own_residual = lax.dynamic_slice_in_dim(residual, column_start, column_count, 1).astype(
        jnp.float32
    )
    layer_out = (own_residual + mixture).astype(jnp.bfloat16)
    return (layer_out, new_state)


def solution(mesh):
    in_specs = (
        P("ep", None),
        P("ep", "tp", None, None),
        P(None, "tp"),
        P(None, "tp"),
        P(None, "tp"),
        P(),
        P(None, "tp"),
        P("tp"),
        P(),
        P(None, "tp"),
        P("tp"),
        P("tp"),
        P("tp", None),
        P("ep", None),
        P("ep", None),
        P("ep", None, "tp"),
        P("ep", None, "tp"),
        P("ep", "tp", None),
    )
    out_specs = (P("ep", "tp"), P("ep", "tp", None, None))
    return jax.shard_map(local, mesh=mesh, in_specs=in_specs, out_specs=out_specs, check_vma=False)
```
